32 devices in a mesh: row: 8 (over z, x), col: 4 (over y, core).
Axes of the slice: x: 2, y: 2, z: 4, core: 2. Of those that a mesh axis runs over, the one named last changes fastest.
Arguments:
- tokens: bfloat16 [9216, 4096], P('row'), may hold values from -6 to 6
- proj_in: bfloat16 [4096, 512], P(None, 'col'), may hold values from -0.09375 to 0.09375
- proj_out: bfloat16 [512, 4096], P(None, 'col'), may hold values from -0.25 to 0.25
Outputs:
- mixed: bfloat16 [9216, 4096], P('row', 'col')
The draws below stay inside these ranges and needn't reach their ends.
All inputs are finite; a program needn't handle non-finite values.
Results may differ from the reference program's by a relative error of at most 0.0057.
Values may be sent and summed in bfloat16 or wider, within the bound.
A program may use at most 64 MiB of HBM per device.

```python
import jax
import jax.numpy as jnp

D = 4096
GW = 128
SEQ = 9216
FW = 512
N_COL = 4


def levels(key, dims, cuts, low, high):
    factor_of, own = 1.0, jax.random.fold_in(key, 6)
    for position, parts in cuts:
        steps = jnp.exp(jax.random.uniform(jax.random.fold_in(own, position), (parts,), jnp.float32, low / len(cuts), high / len(cuts)))
        factor_of = factor_of * jnp.repeat(steps, dims[position] // parts).reshape([-1 if axis == position else 1 for axis in range(len(dims))])
    return factor_of


def centred(rng, dims, width, limit, pieces=(), kind=jnp.bfloat16):
    gain = levels(rng, dims, pieces, -0.22, 0.18) if pieces else 1.0
    result = jax.random.normal(rng, dims, jnp.float32) * width * gain
    return jnp.minimum(jnp.maximum(result, -limit), limit).astype(kind)


def setup_inputs(seed: int = 0) -> dict:
    key_of = jax.random.split(jax.random.key(seed), 4)
    tokens = centred(key_of[0], (SEQ, D), 1.0, 6.0, ((0, 8),))
    proj_in = centred(key_of[1], (D, FW), D ** -0.5, 0.09375, ((1, 4),))
    proj_out = centred(key_of[2], (FW, D), FW ** -0.5, 0.25, ((1, 4),))
    return dict(tokens=tokens, proj_in=proj_in, proj_out=proj_out)


def reference(tokens, proj_in, proj_out):
    branch_in = jnp.dot(tokens, proj_in, preferred_element_type=jnp.float32).astype(jnp.bfloat16)
    grouped = branch_in.astype(jnp.float32).reshape(SEQ, N_COL, GW)
    spectrum = jnp.fft.fft2(grouped, axes=(0, 2), norm="ortho").real
    spectrum = spectrum.astype(jnp.bfloat16).reshape(SEQ, FW)
    return jnp.dot(spectrum, proj_out, preferred_element_type=jnp.float32).astype(jnp.bfloat16)
```

```python
import functools
import math

import jax
import jax.numpy as jnp
import numpy as np
from jax import lax
from jax.experimental import pallas as pl
from jax.experimental.pallas import tpu as pltpu
from jax.sharding import PartitionSpec as P

MESH = pl.DeviceIdType.MESH


def up(value, step):
    return -(-value // step) * step


def plan(rows, devices):
    period = rows // 2
    piece = rows // (2 * devices)
    pad = up(piece, 8)
    share = period // (2 * devices)
    height = up(share + 1, 8)
    return period, piece, pad, share, height


@functools.lru_cache(maxsize=None)
def tables(rows, devices, group):
    period, piece, pad, share, height = plan(rows, devices)
    half = group // 2
    odd = np.arange(group) > half
    freq = np.where(odd, np.arange(group) - half, np.arange(group))
    angle = 2 * np.pi * (np.arange(group)[:, None] * freq[None, :] % group) / group
    chan = np.where(odd, np.sin(angle), np.cos(angle)) / math.sqrt(group)
    chan_hi = chan.astype(jnp.bfloat16)
    chan_lo = (chan - chan_hi.astype(np.float64)).astype(jnp.bfloat16)
    unpack = np.zeros((group, group))
    for col in range(group):
        f = freq[col]
        unpack[col, f] = -1.0 if odd[col] else 1.0
        unpack[col, (group - f) % group] = 1.0
    pos = np.arange(2 * pad)
    is_y = pos >= pad
    local = np.where(is_y, pos - pad, pos)
    valid = np.tile(local < piece, devices)
    m = (piece * np.arange(devices)[:, None] + local[None, :]).reshape(-1)
    is_y = np.tile(is_y, devices)
    k = (share * np.arange(devices)[:, None] + np.arange(height)[None, :])
    pair_m = 2 * np.where(is_y, period - 1 - m, m)
    self_m = 2 * m + is_y
    seq = []
    for twice_m in (self_m, pair_m):
        angle = np.pi * (twice_m[None, None, :] * k[:, :, None] % (2 * period)) / period
        both = np.stack([np.cos(angle), np.sin(angle)], axis=1) * valid
        seq.append(both.reshape(devices * 2 * height, -1))
    seq = np.stack(seq).astype(jnp.bfloat16)
    q = np.arange(2 * devices)[:, None]
    p = np.arange(devices)[None, :]
    angle = 2 * np.pi * (p * q % (2 * devices)) / (2 * devices)
    even_a, even_b = np.cos(angle), -np.sin(angle)
    odd_a, odd_b = np.sin(angle), np.cos(angle)
    for a, b in ((even_a, even_b), (odd_a, odd_b)):
        a[:, 0] = 1.0
        b[:, 0] = np.where(q[:, 0] % 2, -1.0, 1.0)
    even = np.stack([even_a, even_b], axis=2).reshape(2 * devices, 2 * devices, 1)
    oddc = np.stack([odd_a, odd_b], axis=2).reshape(2 * devices, 2 * devices, 1)
    coef = np.where(odd, oddc, even) / math.sqrt(rows * devices)
    order = np.zeros((period, devices * 2 * height))
    for row in range(period):
        mirrored = row > period // 2
        kk = period - row if mirrored else row
        s = min(kk // share, devices - 1)
        order[row, s * 2 * height + mirrored * height + kk - s * share] = 1.0
    return (
        np.stack([chan_hi, chan_lo]),
        unpack.astype(jnp.bfloat16),
        seq,
        coef.astype(np.float32),
        order.astype(jnp.bfloat16),
    )


def cos_sin_small(x):
    square = x * x
    cos_sum, sin_sum = jnp.zeros_like(x), jnp.zeros_like(x)
    for j in range(8, -1, -1):
        sign = -1.0 if j % 2 else 1.0
        cos_sum = cos_sum * square + sign / math.factorial(2 * j)
        sin_sum = sin_sum * square + sign / math.factorial(2 * j + 1)
    return cos_sum, sin_sum * x


def kernel(
    devices, cols, chunks,
    tok_hbm, pin_hbm, pout_hbm, chan_hbm, unpack_hbm, seq_hbm, coef_hbm, order_hbm,
    out_ref,
    tok, pin, pout, chan, unpack, seq, coef, order,
    packed, wide, slot1, send1, recv1, mid, send2, recv2, twc, tws, parts, send3, recv3, weight,
    tok_sem, in_sem, ssem1, rsem1, ssem2, rsem2, ssem3, rsem3, gsem, ysem, psem,
):
    me = lax.axis_index("row")
    col = lax.axis_index("col")
    partner = col + 1 - 2 * lax.rem(col, 2)
    rows, group = packed.shape
    period, piece, pad, share, height = plan(rows, devices)
    half = group // 2
    f32, bf16 = jnp.float32, jnp.bfloat16
    chips = cols // 2

    def peer_row(d):
        return lax.rem(me + d, devices)

    def peer_col(j):
        return lax.rem(col + 2 * j, cols)

    barrier = pltpu.get_barrier_semaphore()

    step = rows // chunks
    tok_copies = [
        pltpu.make_async_copy(
            tok_hbm.at[pl.ds(i * step, step)], tok.at[pl.ds(i * step, step)], tok_sem.at[i]
        )
        for i in range(chunks)
    ]
    loads = [
        pltpu.make_async_copy(src, dst, in_sem.at[i])
        for i, (src, dst) in enumerate(
            [
                (pin_hbm, pin),
                (chan_hbm, chan),
                (seq_hbm.at[jnp.minimum(me, 1)], seq),
                (pout_hbm, pout),
                (unpack_hbm, unpack),
                (coef_hbm, coef),
                (order_hbm, order),
            ]
        )
    ]
    loads[0].start()
    loads[1].start()
    for copy in tok_copies:
        copy.start()
    for copy in loads[2:]:
        copy.start()

    def greet(d, _):
        pl.semaphore_signal(barrier, inc=1, device_id={"row": peer_row(d)}, device_id_type=MESH)
        return 0

    lax.fori_loop(1, devices, greet, 0)
    pl.semaphore_signal(barrier, inc=1, device_id={"col": partner}, device_id_type=MESH)
    for j in range(1, chips):
        pl.semaphore_signal(barrier, inc=1, device_id={"col": peer_col(j)}, device_id_type=MESH)

    shape = (devices, height, group)
    p_id = lax.broadcasted_iota(jnp.int32, shape, 0)
    k_id = lax.broadcasted_iota(jnp.int32, shape, 1) + share * me
    angle = (p_id * k_id).astype(f32) * (2.0 * math.pi / (rows * devices))
    cos_val, sin_val = cos_sin_small(angle)
    twc[...] = cos_val
    tws[...] = sin_val

    lane = lax.broadcasted_iota(jnp.int32, (1, group), 1)
    sign = jnp.where(lane > half, -1.0, 1.0).astype(f32)

    loads[0].wait()
    loads[1].wait()
    for i in range(chunks):
        tok_copies[i].wait()
        branch = jnp.dot(
            tok[i * step:(i + 1) * step, :], pin[...], preferred_element_type=f32
        ).astype(bf16)
        packed[i * step:(i + 1) * step, :] = jnp.dot(
            branch, chan[0], preferred_element_type=f32
        ) + jnp.dot(branch, chan[1], preferred_element_type=f32)

    pl.semaphore_wait(barrier, devices - 1 + 1 + chips - 1)

    if pad != piece:
        slot1[...] = jnp.zeros_like(slot1)
    for p in range(devices):
        other = 2 * devices - p if p else devices
        x = packed[pl.ds(p, piece, stride=2 * devices), :]
        y = packed[pl.ds(other, piece, stride=2 * devices), :]
        if p:
            y = y * sign
        if pad == piece:
            send1[p] = jnp.concatenate([x, y], axis=0).astype(bf16)
        else:
            slot1[0:piece, :] = x
            slot1[pad:pad + piece, :] = y
            send1[p] = slot1[...].astype(bf16)

    def remote(src, dst, ssem, rsem, target):
        return pltpu.make_async_remote_copy(
            src_ref=src, dst_ref=dst, send_sem=ssem, recv_sem=rsem,
            device_id=target, device_id_type=MESH,
        )

    def exchange1(d, slot):
        to = peer_row(d)
        return remote(send1.at[to], recv1.at[slot], ssem1.at[d], rsem1.at[slot], {"row": to})

    def start1(d, _):
        exchange1(d, me).start()
        return 0

    lax.fori_loop(1, devices, start1, 0)
    recv1[me] = send1[me]

    for copy in loads[2:]:
        copy.wait()
    for c in range(cols):
        weight[c * group:(c + 1) * group, :] = jnp.dot(
            unpack[...], pout[c * group:(c + 1) * group, :], preferred_element_type=f32
        ).astype(bf16)

    def wait1(d, _):
        exchange1(d, lax.rem(me + devices - d, devices)).wait_recv()
        return 0

    lax.fori_loop(1, devices, wait1, 0)

    data = recv1[...].astype(f32)
    is_y = lax.broadcasted_iota(jnp.int32, data.shape, 1) >= pad
    flat = (devices * 2 * pad, group)
    both = jnp.concatenate(
        [
            jnp.where(is_y, 0.0, data).astype(bf16).reshape(flat),
            jnp.where(is_y, data, 0.0).astype(bf16).reshape(flat),
        ],
        axis=1,
    )
    mid[...] = jnp.dot(seq[...], both, preferred_element_type=f32).reshape(mid.shape)
    first = me == 0
    odd_lane = lane > half

    def exchange2(d, slot):
        to = peer_row(d)
        return remote(send2.at[to], recv2.at[slot], ssem2.at[d], rsem2.at[slot], {"row": to})

    def start2(d, _):
        s = peer_row(d)
        top_x, top_y = mid[s, :height, :group], mid[s, :height, group:]
        low_x, low_y = mid[s, height:, :group], mid[s, height:, group:]
        a = jnp.where(first, jnp.where(odd_lane, low_x, top_x), top_x + top_y)
        b = jnp.where(first, jnp.where(odd_lane, low_y, top_y), low_x + low_y)
        send2[s] = jnp.concatenate([a, b], axis=0).astype(bf16)

        @pl.when(d < devices)
        def _():
            exchange2(d, me).start()

        return 0

    lax.fori_loop(1, devices + 1, start2, 0)
    recv2[me] = send2[me]

    def rotate(p):
        ab = recv2[p].astype(f32)
        a, b = ab[:height], ab[height:]
        cos_val, sin_val = twc[p], tws[p]
        parts[2 * p] = cos_val * a - sin_val * b
        parts[2 * p + 1] = sin_val * a + cos_val * b

    rotate(me)

    def wait2(d, _):
        src = lax.rem(me + devices - d, devices)
        exchange2(d, src).wait_recv()
        rotate(src)
        return 0

    lax.fori_loop(1, devices, wait2, 0)

    def exchange3(to, slot):
        return remote(send3.at[to], recv3.at[col, slot], ssem3.at[to], rsem3.at[slot], {"row": to})

    def outer(q):
        return jnp.sum(coef[q][:, None, :] * parts[...], axis=0)

    def send_to(to):
        @pl.when(to != me)
        def _():
            exchange3(to, me).start()

    def start3(i, _):
        for h in range(2):
            q = 2 * i + h
            direct = outer(q)
            mirror = outer(2 * devices - 1 - q)
            send3[i, h] = jnp.concatenate([direct, mirror * sign], axis=0).astype(bf16)
            send3[devices - 1 - i, 1 - h] = jnp.concatenate(
                [mirror, direct * sign], axis=0
            ).astype(bf16)
        send_to(i)
        send_to(devices - 1 - i)
        return 0

    lax.fori_loop(0, devices // 2, start3, 0)
    recv3[col, me] = send3[me]

    def to_partner(c, src):
        block = recv3.at[c, src]
        return remote(block, block, psem.at[c, src], gsem.at[c, src], {"col": partner})

    def to_chip(j, c, src):
        block = recv3.at[c, src]
        return remote(block, block, ysem.at[j, src], gsem.at[c, src], {"col": peer_col(j)})

    def forward(src):
        for j in range(1, chips):
            to_chip(j, col, src).start()
        to_partner(col, src).start()

    def relay(src):
        for j in range(1, chips):
            c = lax.rem(col + cols - 2 * j, cols)
            to_chip(j, c, src).wait_recv()
            to_partner(c, src).start()

    forward(me)

    def wait3(d, _):
        src = lax.rem(me + devices - d, devices)
        pltpu_wait = remote(
            send3.at[me], recv3.at[col, src], ssem3.at[me], rsem3.at[src], {"row": src}
        )
        pltpu_wait.wait_recv()
        forward(src)
        return 0

    lax.fori_loop(1, devices, wait3, 0)

    def relay_all(d, _):
        relay(lax.rem(me + devices - d, devices))
        return 0

    lax.fori_loop(0, devices, relay_all, 0)

    def wait_partner(d, _):
        src = lax.rem(me + devices - d, devices)
        for j in range(chips):
            c = lax.rem(partner + 2 * j, cols)
            to_partner(c, src).wait_recv()
        return 0

    lax.fori_loop(0, devices, wait_partner, 0)

    for h in range(2):
        arrived = jnp.concatenate(
            [recv3[c, :, h].reshape(devices * 2 * height, group) for c in range(cols)], axis=1
        )
        natural = jnp.dot(order[...], arrived, preferred_element_type=f32).astype(bf16)
        out_ref[h * period:(h + 1) * period, :] = jnp.dot(
            natural, weight[...], preferred_element_type=f32
        ).astype(bf16)

    def drain(d, _):
        exchange1(d, me).wait_send()
        exchange2(d, me).wait_send()
        exchange3(peer_row(d), me).wait_send()
        return 0

    lax.fori_loop(1, devices, drain, 0)

    def drain_gather(src, _):
        for j in range(1, chips):
            to_chip(j, col, src).wait_send()
        for j in range(chips):
            to_partner(peer_col(j), src).wait_send()
        return 0

    lax.fori_loop(0, devices, drain_gather, 0)


def solution(mesh):
    devices, cols = mesh.shape["row"], mesh.shape["col"]

    def on_device(tokens, proj_in, proj_out):
        rows, width = tokens.shape
        group = proj_in.shape[1]
        channels, out_cols = proj_out.shape
        period, piece, pad, share, height = plan(rows, devices)
        consts = tables(rows, devices, group)
        chunks = 8
        f32, bf16 = jnp.float32, jnp.bfloat16
        dma = pltpu.SemaphoreType.DMA
        seq_shape = consts[2].shape[1:]
        return pl.pallas_call(
            functools.partial(kernel, devices, cols, chunks),
            out_shape=jax.ShapeDtypeStruct((rows, out_cols), bf16),
            in_specs=[pl.BlockSpec(memory_space=pltpu.HBM)] * 8,
            out_specs=pl.BlockSpec(memory_space=pltpu.VMEM),
            scratch_shapes=[
                pltpu.VMEM((rows, width), bf16),
                pltpu.VMEM((width, group), bf16),
                pltpu.VMEM((channels, out_cols), bf16),
                pltpu.VMEM((2, group, group), bf16),
                pltpu.VMEM((group, group), bf16),
                pltpu.VMEM(seq_shape, bf16),
                pltpu.VMEM((2 * devices, 2 * devices, group), f32),
                pltpu.VMEM(consts[4].shape, bf16),
                pltpu.VMEM((rows, group), f32),
                pltpu.VMEM((8, group), f32),
                pltpu.VMEM((2 * pad, group), f32),
                pltpu.VMEM((devices, 2 * pad, group), bf16),
                pltpu.VMEM((devices, 2 * pad, group), bf16),
                pltpu.VMEM((devices, 2 * height, 2 * group), f32),
                pltpu.VMEM((devices, 2 * height, group), bf16),
                pltpu.VMEM((devices, 2 * height, group), bf16),
                pltpu.VMEM((devices, height, group), f32),
                pltpu.VMEM((devices, height, group), f32),
                pltpu.VMEM((2 * devices, height, group), f32),
                pltpu.VMEM((devices, 2, 2 * height, group), bf16),
                pltpu.VMEM((cols, devices, 2, 2 * height, group), bf16),
                pltpu.VMEM((channels, out_cols), bf16),
                dma((chunks,)),
                dma((7,)),
                dma((devices,)),
                dma((devices,)),
                dma((devices,)),
                dma((devices,)),
                dma((devices,)),
                dma((devices,)),
                dma((cols, devices)),
                dma((cols // 2, devices)),
                dma((cols, devices)),
            ],
            compiler_params=pltpu.CompilerParams(
                collective_id=0, has_side_effects=True, vmem_limit_bytes=40 * 2**20
            ),
            name="mix",
        )(*[pltpu.with_memory_space_constraint(a, pltpu.HBM) for a in (tokens, proj_in, proj_out, *[jnp.asarray(c) for c in consts])])

    return jax.shard_map(
        on_device,
        mesh=mesh,
        in_specs=(P("row", None), P(None, "col"), P(None, "col")),
        out_specs=P("row", "col"),
        check_vma=False,
    )
```

```python
import functools
import math

import jax
import jax.numpy as jnp
import numpy as np
from jax import lax
from jax.experimental import pallas as pl
from jax.experimental.pallas import tpu as pltpu
from jax.sharding import PartitionSpec as P

MESH = pl.DeviceIdType.MESH


def up(value, step):
    return -(-value // step) * step


def plan(rows, devices):
    period = rows // 2
    piece = rows // (2 * devices)
    subs = 3 if piece % 24 == 0 else 1
    pad = up(piece // subs, 8)
    share = period // (2 * devices)
    height = up(share + 1, 8)
    packet = up(2 * share, 8)
    return period, piece, subs, pad, share, height, packet


@functools.lru_cache(maxsize=None)
def tables(rows, devices, group):
    period, piece, subs, pad, share, height, packet = plan(rows, devices)
    half = group // 2
    odd = np.arange(group) > half
    freq = np.where(odd, np.arange(group) - half, np.arange(group))
    angle = 2 * np.pi * (np.arange(group)[:, None] * freq[None, :] % group) / group
    chan = np.where(odd, np.sin(angle), np.cos(angle)) / math.sqrt(group)
    chan_hi = chan.astype(jnp.bfloat16)
    chan_lo = (chan - chan_hi.astype(np.float64)).astype(jnp.bfloat16)
    unpack = np.zeros((group, group))
    for col in range(group):
        f = freq[col]
        unpack[col, f] = -1.0 if odd[col] else 1.0
        unpack[col, (group - f) % group] = 1.0
    part = piece // subs
    pos = np.arange(2 * pad)
    is_y = pos >= pad
    local = np.where(is_y, pos - pad, pos)
    valid = np.tile(local < part, devices * subs)
    m = (part * np.arange(devices * subs)[:, None] + local[None, :]).reshape(-1)
    is_y = np.tile(is_y, devices * subs)
    k = share * np.arange(devices)[:, None] + np.arange(height)[None, :]
    seq = []
    for twice_m in (2 * m + is_y, 2 * np.where(is_y, period - 1 - m, m)):
        angle = np.pi * (twice_m[None, None, :] * k[:, :, None] % (2 * period)) / period
        both = np.stack([np.cos(angle), np.sin(angle)], axis=1) * valid
        seq.append(both.reshape(devices * 2 * height, -1))
    seq = np.stack(seq).astype(jnp.bfloat16)
    q = np.arange(2 * devices)[:, None]
    p = np.arange(devices)[None, :]
    angle = 2 * np.pi * (p * q % (2 * devices)) / (2 * devices)
    even_a, even_b = np.cos(angle), -np.sin(angle)
    odd_a, odd_b = np.sin(angle), np.cos(angle)
    for a, b in ((even_a, even_b), (odd_a, odd_b)):
        a[:, 0] = 1.0
        b[:, 0] = np.where(q[:, 0] % 2, -1.0, 1.0)
    coef = []
    for c in range(2):
        is_odd = odd[c * half:(c + 1) * half]
        first = np.where(is_odd, odd_a[:, :, None], even_a[:, :, None])
        second = np.where(is_odd, odd_b[:, :, None], even_b[:, :, None])
        coef.append(np.concatenate([first, second], axis=2))
    coef = np.stack(coef) / math.sqrt(rows * devices)
    perm = np.zeros((packet, 2 * height))
    for j in range(share):
        perm[j, j] = 1.0
        perm[share + j, height + share - j] = 1.0
    order = np.zeros((period, devices * packet))
    for row in range(period):
        if row < period // 2:
            order[row, row // share * packet + row % share] = 1.0
        else:
            s = (period - 1 - row) // share
            order[row, s * packet + share + row - (period - share * (s + 1))] = 1.0
    return (
        np.concatenate([chan_hi, chan_lo], axis=0),
        unpack.astype(jnp.bfloat16),
        seq,
        coef.astype(np.float32),
        perm.astype(jnp.bfloat16),
        order.astype(jnp.bfloat16),
    )


def cos_sin_small(x):
    square = x * x
    cos_sum, sin_sum = jnp.zeros_like(x), jnp.zeros_like(x)
    for j in range(8, -1, -1):
        sign = -1.0 if j % 2 else 1.0
        cos_sum = cos_sum * square + sign / math.factorial(2 * j)
        sin_sum = sin_sum * square + sign / math.factorial(2 * j + 1)
    return cos_sum, sin_sum * x


def kernel(
    devices, cols, chunks,
    tok_hbm, pin_hbm, pout_hbm, chan_hbm, unpack_hbm, seq_hbm, coef_hbm, perm_hbm, order_hbm,
    out_ref,
    tok, pin, pout, chan, unpack, seq, coef, perm, order,
    packed, send1, recv1, mid, send2, recv2, twc, tws, parts, send3, recv3, weight, acc,
    tok_sem, in_sem, ssem1, rsem1, ssem2, rsem2, ssem3, rsem3, gsem, ysem, psem,
):
    me = lax.axis_index("row")
    col = lax.axis_index("col")
    partner = col + 1 - 2 * lax.rem(col, 2)
    rows, group = packed.shape
    period, piece, subs, pad, share, height, packet = plan(rows, devices)
    half = group // 2
    f32, bf16 = jnp.float32, jnp.bfloat16
    chips = cols // 2
    wing = devices // 2

    def target(d):
        return lax.rem(me + 1 + d, devices)

    def source(d):
        return lax.rem(me + devices - 1 - d, devices)

    def peer_col(j):
        return lax.rem(col + 2 * j, cols)

    def each(body, count=devices - 1):
        def step(d, _):
            body(d)
            return 0

        lax.fori_loop(0, count, step, 0)

    barrier = pltpu.get_barrier_semaphore()

    step = rows // chunks
    depth = chunks // 2
    tok_copies = [
        pltpu.make_async_copy(
            tok_hbm.at[pl.ds(i * step, step)], tok.at[pl.ds(i * step, step)], tok_sem.at[i]
        )
        for i in range(chunks)
    ]
    loads = [
        pltpu.make_async_copy(src, dst, in_sem.at[i])
        for i, (src, dst) in enumerate(
            [
                (pin_hbm, pin),
                (chan_hbm, chan),
                (pout_hbm, pout),
                (unpack_hbm, unpack),
                (seq_hbm.at[jnp.minimum(me, 1)], seq),
                (coef_hbm, coef),
                (perm_hbm, perm),
                (order_hbm, order),
            ]
        )
    ]
    loads[0].start()
    tok_copies[0].start()
    loads[1].start()
    for copy in tok_copies[1:depth]:
        copy.start()
    each(lambda d: pl.semaphore_signal(
        barrier, inc=1, device_id={"row": target(d)}, device_id_type=MESH
    ))
    pl.semaphore_signal(barrier, inc=1, device_id={"col": partner}, device_id_type=MESH)
    for j in range(1, chips):
        pl.semaphore_signal(barrier, inc=1, device_id={"col": peer_col(j)}, device_id_type=MESH)

    lane = lax.broadcasted_iota(jnp.int32, (1, group), 1)
    low = lane < half

    shape = (devices, height, group)
    p_id = lax.broadcasted_iota(jnp.int32, shape, 0)
    k_id = lax.broadcasted_iota(jnp.int32, shape, 1) + share * me
    angle = (p_id * k_id).astype(f32) * (2.0 * math.pi / (rows * devices))
    cos_val, sin_val = cos_sin_small(angle)
    twc[...] = cos_val
    tws[...] = jnp.where(low, -sin_val, sin_val)

    def sign_of(channel):
        return jnp.where(channel > half, -1.0, 1.0).astype(f32)

    y_sign = sign_of(lane)

    def remote(src, dst, ssem, rsem, to):
        return pltpu.make_async_remote_copy(
            src_ref=src, dst_ref=dst, send_sem=ssem, recv_sem=rsem,
            device_id=to, device_id_type=MESH,
        )

    def exchange1(r, to, slot):
        return remote(
            send1.at[r, to], recv1.at[slot, r], ssem1.at[r, to], rsem1.at[r, slot], {"row": to}
        )

    part = piece // subs
    per_sub = chunks // subs
    if pad != part:
        send1[...] = jnp.zeros_like(send1)
    loads[0].wait()
    for i in range(chunks):
        tok_copies[i].wait()
        if i + depth < chunks:
            tok_copies[i + depth].start()
        elif i + depth == chunks:
            for copy in loads[2:]:
                copy.start()
        branch = jnp.dot(
            tok[i * step:(i + 1) * step, :], pin[...], preferred_element_type=f32
        ).astype(bf16)
        if i == 0:
            loads[1].wait()
        packed[i * step:(i + 1) * step, :] = jnp.dot(
            jnp.concatenate([branch, branch], axis=1), chan[...], preferred_element_type=f32
        )
        if (i + 1) % per_sub:
            continue
        r = i // per_sub
        base = r * (rows // subs)
        for p in range(devices):
            other = 2 * devices - p if p else devices
            y = packed[pl.ds(base + other, part, stride=2 * devices), :]
            if p:
                y = y * y_sign
            x = packed[pl.ds(base + p, part, stride=2 * devices), :]
            send1[r, p, 0, 0:part, :] = x.astype(bf16)
            send1[r, p, 1, 0:part, :] = y.astype(bf16)
        if r == 0:
            pl.semaphore_wait(barrier, devices - 1 + 1 + chips - 1)
        each(lambda d: exchange1(r, target(d), me).start())
    for r in range(subs):
        recv1[me, r] = send1[r, me]

    for copy in loads[2:]:
        copy.wait()
    for g in range(cols):
        unpacked = jnp.dot(
            unpack[...], pout[g * group:(g + 1) * group, :], preferred_element_type=f32
        ).astype(bf16)
        top = g // 2 * group
        for v in range(2):
            at = top + (half if (g + v) % 2 else 0)
            for c in range(2):
                weight[v, c, at:at + half, :] = unpacked[c * half:(c + 1) * half, :]

    first = me == 0

    def exchange2(c, to, slot):
        return remote(
            send2.at[c, to], recv2.at[c, slot], ssem2.at[c, to], rsem2.at[c, slot], {"row": to}
        )

    def channel_of(c):
        return c * half + lax.rem(lane, half)

    odd_lane = lane > half
    for r in range(subs):
        each(lambda d: exchange1(r, me, source(d)).wait_recv())
    data = recv1[...].reshape(devices * subs, 2, pad, group)
    blank = jnp.zeros_like(data[:, 0])
    flat = (devices * subs * 2 * pad, group)
    both = jnp.concatenate(
        [
            jnp.stack([data[:, 0], blank], axis=1).reshape(flat),
            jnp.stack([blank, data[:, 1]], axis=1).reshape(flat),
        ],
        axis=1,
    )
    mid[...] = jnp.dot(seq[...], both, preferred_element_type=f32).reshape(mid.shape)

    def fill(s):
        top_x, top_y = mid[s, :height, :group], mid[s, :height, group:]
        low_x, low_y = mid[s, height:, :group], mid[s, height:, group:]
        a = jnp.where(first, jnp.where(odd_lane, low_x, top_x), top_x + top_y)
        b = jnp.where(first, jnp.where(odd_lane, low_y, top_y), low_x + low_y)
        send2[0, s] = jnp.where(low, a, pltpu.roll(b, half, 1)).astype(bf16)
        send2[1, s] = jnp.where(low, pltpu.roll(a, half, 1), b).astype(bf16)

    def start2(d):
        fill(target(d))
        exchange2(0, target(d), me).start()

    each(start2)
    each(lambda d: exchange2(1, target(d), me).start())
    fill(me)
    recv2[0, me] = send2[0, me]
    recv2[1, me] = send2[1, me]

    def exchange3(c, to, slot):
        return remote(
            send3.at[c, to], recv3.at[c, col, slot], ssem3.at[c, to], rsem3.at[c, slot],
            {"row": to},
        )

    keep = jnp.logical_xor(low, lax.rem(col, 2) == 1)

    def combine(c):
        def rotate(src):
            value = recv2[c, src].astype(f32)
            parts[src] = twc[src] * value + tws[src] * pltpu.roll(value, half, 1)

        rotate(me)

        def arrive(d):
            exchange2(c, me, source(d)).wait_recv()
            rotate(source(d))

        each(arrive)
        sign = sign_of(channel_of(c))

        def outer(q):
            total = coef[c, q, 0][None, :] * parts[0]
            for p in range(1, devices):
                total = total + coef[c, q, p][None, :] * parts[p]
            return total

        def merge(one, two):
            return jnp.where(keep, one, two) + pltpu.roll(jnp.where(keep, two, one), half, 1)

        def pair(i):
            here = merge(outer(2 * i), outer(2 * i + 1))
            there = merge(outer(2 * devices - 1 - 2 * i), outer(2 * devices - 2 - 2 * i))
            stacked = jnp.concatenate(
                [
                    jnp.concatenate([here, there * sign], axis=0),
                    jnp.concatenate([there, here * sign], axis=0),
                ],
                axis=1,
            ).astype(bf16)
            moved = jnp.dot(perm[...], stacked, preferred_element_type=f32).astype(bf16)
            send3[c, i] = moved[:, :group]
            send3[c, devices - 1 - i] = moved[:, group:]

        if devices <= 8:
            for i in range(wing):
                pair(i)
        else:
            each(pair, wing)
        each(lambda d: exchange3(c, target(d), me).start())
        recv3[c, col, me] = send3[c, me]

    combine(0)
    combine(1)

    def to_partner(c, g, src):
        block = recv3.at[c, g, src]
        return remote(block, block, psem.at[g, src], gsem.at[c, g, src], {"col": partner})

    def to_chip(c, j, g, src):
        block = recv3.at[c, g, src]
        return remote(block, block, ysem.at[j, src], gsem.at[c, g, src], {"col": peer_col(j)})

    def forward(c, src):
        for j in range(1, chips):
            if c:
                to_chip(0, j, col, src).wait_send()
            to_chip(c, j, col, src).start()
        if c:
            to_partner(0, col, src).wait_send()
        to_partner(c, col, src).start()

    def relay(c, src):
        for j in range(1, chips):
            g = lax.rem(col + cols - 2 * j, cols)
            to_chip(c, j, g, src).wait_recv()
            if c:
                to_partner(0, g, src).wait_send()
            to_partner(c, g, src).start()

    def pass_on(c, src):
        exchange3(c, me, src).wait_recv()
        forward(c, src)

    def collect(c, src):
        for j in range(chips):
            to_partner(c, lax.rem(partner + 2 * j, cols), src).wait_recv()

    upper = me // wing
    mine = jnp.logical_xor(low, upper == 1)

    def finish(c, h):
        tiles = []
        for t in range(chips):
            one = recv3[c, 2 * t].reshape(devices * packet, group)
            two = recv3[c, 2 * t + 1].reshape(devices * packet, group)
            tiles.append(jnp.where(mine, two, one) if h else jnp.where(mine, one, two))
        arrived = jnp.concatenate(tiles, axis=1) if chips > 1 else tiles[0]
        natural = jnp.dot(order[...], arrived, preferred_element_type=f32).astype(bf16)
        which = 1 - upper if h else upper
        part = jnp.dot(natural, weight[which, c], preferred_element_type=f32)
        at = slice(h * period, (h + 1) * period)
        if c == 0:
            acc[at, :] = part
        else:
            out_ref[at, :] = (acc[at, :] + part).astype(bf16)

    forward(0, me)
    each(lambda d: pass_on(0, source(d)))
    forward(1, me)
    relay(0, me)

    def second(d):
        pass_on(1, source(d))
        relay(0, source(d))

    each(second)
    collect(0, me)
    each(lambda d: collect(0, source(d)))
    finish(0, 0)
    relay(1, me)
    each(lambda d: relay(1, source(d)))
    finish(0, 1)
    collect(1, me)
    each(lambda d: collect(1, source(d)))
    finish(1, 0)
    finish(1, 1)

    def drain(d):
        to = target(d)
        for r in range(subs):
            exchange1(r, to, me).wait_send()
        for c in range(2):
            exchange2(c, to, me).wait_send()
            exchange3(c, to, me).wait_send()

    each(drain)

    def drain_gather(src):
        for j in range(1, chips):
            to_chip(1, j, col, src).wait_send()
        for j in range(chips):
            to_partner(1, peer_col(j), src).wait_send()

    each(drain_gather, devices)


def solution(mesh):
    devices, cols = mesh.shape["row"], mesh.shape["col"]

    def on_device(tokens, proj_in, proj_out):
        rows, width = tokens.shape
        group = proj_in.shape[1]
        channels, out_cols = proj_out.shape
        period, piece, subs, pad, share, height, packet = plan(rows, devices)
        consts = tables(rows, devices, group)
        chunks = 6
        f32, bf16 = jnp.float32, jnp.bfloat16
        dma = pltpu.SemaphoreType.DMA
        operands = [tokens, proj_in, proj_out, *[jnp.asarray(c) for c in consts]]
        return pl.pallas_call(
            functools.partial(kernel, devices, cols, chunks),
            out_shape=jax.ShapeDtypeStruct((rows, out_cols), bf16),
            in_specs=[pl.BlockSpec(memory_space=pltpu.HBM)] * len(operands),
            out_specs=pl.BlockSpec(memory_space=pltpu.VMEM),
            scratch_shapes=[
                pltpu.VMEM((rows, width), bf16),
                pltpu.VMEM((width, group), bf16),
                pltpu.VMEM((channels, out_cols), bf16),
                pltpu.VMEM(consts[0].shape, bf16),
                pltpu.VMEM((group, group), bf16),
                pltpu.VMEM(consts[2].shape[1:], bf16),
                pltpu.VMEM(consts[3].shape, f32),
                pltpu.VMEM(consts[4].shape, bf16),
                pltpu.VMEM(consts[5].shape, bf16),
                pltpu.VMEM((rows, group), f32),
                pltpu.VMEM((subs, devices, 2, pad, group), bf16),
                pltpu.VMEM((devices, subs, 2, pad, group), bf16),
                pltpu.VMEM((devices, 2 * height, 2 * group), f32),
                pltpu.VMEM((2, devices, height, group), bf16),
                pltpu.VMEM((2, devices, height, group), bf16),
                pltpu.VMEM((devices, height, group), f32),
                pltpu.VMEM((devices, height, group), f32),
                pltpu.VMEM((devices, height, group), f32),
                pltpu.VMEM((2, devices, packet, group), bf16),
                pltpu.VMEM((2, cols, devices, packet, group), bf16),
                pltpu.VMEM((2, 2, channels // 2, out_cols), bf16),
                pltpu.VMEM((rows, out_cols), f32),
                dma((chunks,)),
                dma((8,)),
                dma((subs, devices)),
                dma((subs, devices)),
                dma((2, devices)),
                dma((2, devices)),
                dma((2, devices)),
                dma((2, devices)),
                dma((2, cols, devices)),
                dma((cols // 2, devices)),
                dma((cols, devices)),
            ],
            compiler_params=pltpu.CompilerParams(
                collective_id=0, has_side_effects=True, vmem_limit_bytes=44 * 2**20
            ),
            name="mix",
        )(*[pltpu.with_memory_space_constraint(a, pltpu.HBM) for a in operands])

    return jax.shard_map(
        on_device,
        mesh=mesh,
        in_specs=(P("row", None), P(None, "col"), P(None, "col")),
        out_specs=P("row", "col"),
        check_vma=False,
    )
```

```python
import functools
import math

import jax
import jax.numpy as jnp
import numpy as np
from jax import lax
from jax.experimental import pallas as pl
from jax.experimental.pallas import tpu as pltpu
from jax.sharding import PartitionSpec as P

MESH = pl.DeviceIdType.MESH


def up(value, step):
    return -(-value // step) * step


def plan(rows, devices):
    period = rows // 2
    piece = rows // (2 * devices)
    subs = 3 if piece % 24 == 0 else 1
    pad = up(piece // subs, 8)
    share = period // (2 * devices)
    height = up(share + 1, 8)
    packet = up(2 * share, 8)
    return period, piece, subs, pad, share, height, packet


@functools.lru_cache(maxsize=None)
def tables(rows, devices, group):
    period, piece, subs, pad, share, height, packet = plan(rows, devices)
    half = group // 2
    odd = np.arange(group) > half
    freq = np.where(odd, np.arange(group) - half, np.arange(group))
    angle = 2 * np.pi * (np.arange(group)[:, None] * freq[None, :] % group) / group
    chan = np.where(odd, np.sin(angle), np.cos(angle)) / math.sqrt(group)
    chan_hi = chan.astype(jnp.bfloat16)
    chan_lo = (chan - chan_hi.astype(np.float64)).astype(jnp.bfloat16)
    unpack = np.zeros((group, group))
    for col in range(group):
        f = freq[col]
        unpack[col, f] = -1.0 if odd[col] else 1.0
        unpack[col, (group - f) % group] = 1.0
    part = piece // subs
    pos = np.arange(2 * pad)
    is_y = pos >= pad
    local = np.where(is_y, pos - pad, pos)
    valid = np.tile(local < part, devices * subs)
    m = (
        part * np.arange(subs)[:, None, None]
        + piece * np.arange(devices)[None, :, None]
        + local[None, None, :]
    ).reshape(-1)
    is_y = np.tile(is_y, devices * subs)
    k = share * np.arange(devices)[:, None] + np.arange(height)[None, :]
    seq = []
    for twice_m in (2 * m + is_y, 2 * np.where(is_y, period - 1 - m, m)):
        angle = np.pi * (twice_m[None, None, :] * k[:, :, None] % (2 * period)) / period
        both = np.stack([np.cos(angle), np.sin(angle)], axis=1) * valid
        seq.append(both.reshape(devices * 2 * height, -1))
    seq = np.stack(seq).astype(jnp.bfloat16)
    q = np.arange(2 * devices)[:, None]
    p = np.arange(devices)[None, :]
    angle = 2 * np.pi * (p * q % (2 * devices)) / (2 * devices)
    even_a, even_b = np.cos(angle), -np.sin(angle)
    odd_a, odd_b = np.sin(angle), np.cos(angle)
    for a, b in ((even_a, even_b), (odd_a, odd_b)):
        a[:, 0] = 1.0
        b[:, 0] = np.where(q[:, 0] % 2, -1.0, 1.0)
    coef = []
    for c in range(2):
        is_odd = odd[c * half:(c + 1) * half]
        first = np.where(is_odd, odd_a[:, :, None], even_a[:, :, None])
        second = np.where(is_odd, odd_b[:, :, None], even_b[:, :, None])
        coef.append(np.concatenate([first, second], axis=2))
    coef = np.stack(coef) / math.sqrt(rows * devices)
    perm = np.zeros((packet, 2 * height))
    for j in range(share):
        perm[j, j] = 1.0
        perm[share + j, height + share - j] = 1.0
    order = np.zeros((period, devices * packet))
    for row in range(period):
        if row < period // 2:
            order[row, row // share * packet + row % share] = 1.0
        else:
            s = (period - 1 - row) // share
            order[row, s * packet + share + row - (period - share * (s + 1))] = 1.0
    return (
        np.concatenate([chan_hi, chan_lo], axis=0),
        unpack.astype(jnp.bfloat16),
        seq,
        coef.astype(np.float32),
        perm.astype(jnp.bfloat16),
        order.astype(jnp.bfloat16),
    )


def cos_sin_small(x):
    square = x * x
    cos_sum, sin_sum = jnp.zeros_like(x), jnp.zeros_like(x)
    for j in range(8, -1, -1):
        sign = -1.0 if j % 2 else 1.0
        cos_sum = cos_sum * square + sign / math.factorial(2 * j)
        sin_sum = sin_sum * square + sign / math.factorial(2 * j + 1)
    return cos_sum, sin_sum * x


def kernel(
    devices, cols, chunks,
    tok_hbm, pin_hbm, pout_hbm, chan_hbm, unpack_hbm, seq_hbm, coef_hbm, perm_hbm, order_hbm,
    out_ref,
    tok, pin, pout, chan, unpack, seq, coef, perm, order,
    packed, send1, recv1, mid, send2, recv2, twc, tws, parts, send3, recv3, weight, acc,
    tok_sem, in_sem, ssem1, rsem1, ssem2, rsem2, ssem3, rsem3, gsem, ysem, nsem, psem,
):
    me = lax.axis_index("row")
    col = lax.axis_index("col")
    partner = col + 1 - 2 * lax.rem(col, 2)
    rows, group = packed.shape
    period, piece, subs, pad, share, height, packet = plan(rows, devices)
    half = group // 2
    f32, bf16 = jnp.float32, jnp.bfloat16
    chips = cols // 2
    wing = devices // 2

    def target(d):
        return lax.rem(me + 1 + d, devices)

    def source(d):
        return lax.rem(me + devices - 1 - d, devices)

    def peer_col(j):
        return lax.rem(col + 2 * j, cols)

    def near(row):
        return row // wing == me // wing

    def each(body, count=devices - 1):
        def step(d, _):
            body(d)
            return 0

        lax.fori_loop(0, count, step, 0)

    barrier = pltpu.get_barrier_semaphore()

    step = rows // chunks
    depth = chunks // 2
    tok_copies = [
        pltpu.make_async_copy(
            tok_hbm.at[pl.ds(i * step, step)], tok.at[pl.ds(i * step, step)], tok_sem.at[i]
        )
        for i in range(chunks)
    ]
    loads = [
        pltpu.make_async_copy(src, dst, in_sem.at[i])
        for i, (src, dst) in enumerate(
            [
                (pin_hbm, pin),
                (chan_hbm, chan),
                (pout_hbm, pout),
                (unpack_hbm, unpack),
                (seq_hbm.at[jnp.minimum(me, 1)], seq),
                (coef_hbm, coef),
                (perm_hbm, perm),
                (order_hbm, order),
            ]
        )
    ]
    loads[0].start()
    tok_copies[0].start()
    loads[1].start()
    for copy in tok_copies[1:depth]:
        copy.start()
    each(lambda d: pl.semaphore_signal(
        barrier, inc=1, device_id={"row": target(d)}, device_id_type=MESH
    ))
    pl.semaphore_signal(barrier, inc=1, device_id={"col": partner}, device_id_type=MESH)
    for j in range(1, chips):
        pl.semaphore_signal(barrier, inc=1, device_id={"col": peer_col(j)}, device_id_type=MESH)

    def greet(d):
        @pl.when(near(target(d)))
        def _():
            for j in range(1, chips):
                pl.semaphore_signal(
                    barrier, inc=1, device_id={"row": target(d), "col": peer_col(j)},
                    device_id_type=MESH,
                )

    each(greet)

    lane = lax.broadcasted_iota(jnp.int32, (1, group), 1)
    low = lane < half

    shape = (devices, height, group)
    p_id = lax.broadcasted_iota(jnp.int32, shape, 0)
    k_id = lax.broadcasted_iota(jnp.int32, shape, 1) + share * me
    angle = (p_id * k_id).astype(f32) * (2.0 * math.pi / (rows * devices))
    cos_val, sin_val = cos_sin_small(angle)
    twc[...] = cos_val
    tws[...] = jnp.where(low, -sin_val, sin_val)

    def sign_of(channel):
        return jnp.where(channel > half, -1.0, 1.0).astype(f32)

    y_sign = sign_of(lane)

    def remote(src, dst, ssem, rsem, to):
        return pltpu.make_async_remote_copy(
            src_ref=src, dst_ref=dst, send_sem=ssem, recv_sem=rsem,
            device_id=to, device_id_type=MESH,
        )

    def exchange1(r, to, slot):
        return remote(
            send1.at[r, to], recv1.at[slot, r], ssem1.at[r, to], rsem1.at[r, slot], {"row": to}
        )

    part = piece // subs
    per_sub = chunks // subs
    if pad != part:
        send1[...] = jnp.zeros_like(send1)
    loads[0].wait()
    for i in range(chunks):
        tok_copies[i].wait()
        if i + depth < chunks:
            tok_copies[i + depth].start()
        elif i + depth == chunks:
            for copy in loads[2:]:
                copy.start()
        branch = jnp.dot(
            tok[i * step:(i + 1) * step, :], pin[...], preferred_element_type=f32
        ).astype(bf16)
        if i == 0:
            loads[1].wait()
        packed[i * step:(i + 1) * step, :] = jnp.dot(
            jnp.concatenate([branch, branch], axis=1), chan[...], preferred_element_type=f32
        )
        if (i + 1) % per_sub:
            continue
        r = i // per_sub
        base = r * (rows // subs)
        for p in range(devices):
            other = 2 * devices - p if p else devices
            y = packed[pl.ds(base + other, part, stride=2 * devices), :]
            if p:
                y = y * y_sign
            x = packed[pl.ds(base + p, part, stride=2 * devices), :]
            send1[r, p, 0, 0:part, :] = x.astype(bf16)
            send1[r, p, 1, 0:part, :] = y.astype(bf16)
        if r == 0:
            pl.semaphore_wait(barrier, devices + (chips - 1) * wing)
        each(lambda d: exchange1(r, target(d), me).start())
    for r in range(subs):
        recv1[me, r] = send1[r, me]

    for copy in loads[2:]:
        copy.wait()
    for g in range(cols):
        unpacked = jnp.dot(
            unpack[...], pout[g * group:(g + 1) * group, :], preferred_element_type=f32
        ).astype(bf16)
        top = g // 2 * group
        for v in range(2):
            at = top + (half if (g + v) % 2 else 0)
            for c in range(2):
                weight[v, c, at:at + half, :] = unpacked[c * half:(c + 1) * half, :]

    first = me == 0

    def exchange2(c, to, slot):
        return remote(
            send2.at[c, to], recv2.at[c, slot], ssem2.at[c, to], rsem2.at[c, slot], {"row": to}
        )

    def channel_of(c):
        return c * half + lax.rem(lane, half)

    odd_lane = lane > half
    span = devices * 2 * pad
    for r in range(subs):
        each(lambda d: exchange1(r, me, source(d)).wait_recv())
        data = recv1[:, r]
        blank = jnp.zeros_like(data[:, 0])
        both = jnp.concatenate(
            [
                jnp.stack([data[:, 0], blank], axis=1).reshape(span, group),
                jnp.stack([blank, data[:, 1]], axis=1).reshape(span, group),
            ],
            axis=1,
        )
        term = jnp.dot(
            seq[:, r * span:(r + 1) * span], both, preferred_element_type=f32
        ).reshape(mid.shape)
        mid[...] = mid[...] + term if r else term

    def fill(s):
        top_x, top_y = mid[s, :height, :group], mid[s, :height, group:]
        low_x, low_y = mid[s, height:, :group], mid[s, height:, group:]
        a = jnp.where(first, jnp.where(odd_lane, low_x, top_x), top_x + top_y)
        b = jnp.where(first, jnp.where(odd_lane, low_y, top_y), low_x + low_y)
        send2[0, s] = jnp.where(low, a, pltpu.roll(b, half, 1)).astype(bf16)
        send2[1, s] = jnp.where(low, pltpu.roll(a, half, 1), b).astype(bf16)

    def start2(d):
        fill(target(d))
        exchange2(0, target(d), me).start()

    each(start2)
    each(lambda d: exchange2(1, target(d), me).start())
    fill(me)
    recv2[0, me] = send2[0, me]
    recv2[1, me] = send2[1, me]

    def exchange3(c, to, slot):
        return remote(
            send3.at[c, to], recv3.at[c, col, slot], ssem3.at[c, to], rsem3.at[c, slot],
            {"row": to},
        )

    def direct(c, j, to):
        return remote(
            send3.at[c, to], recv3.at[c, col, me], nsem.at[j, to], gsem.at[c, col, me],
            {"row": to, "col": peer_col(j)},
        )

    keep = jnp.logical_xor(low, lax.rem(col, 2) == 1)

    def combine(c):
        def rotate(src):
            value = recv2[c, src].astype(f32)
            parts[src] = twc[src] * value + tws[src] * pltpu.roll(value, half, 1)

        rotate(me)

        def arrive(d):
            exchange2(c, me, source(d)).wait_recv()
            rotate(source(d))

        each(arrive)
        sign = sign_of(channel_of(c))

        def outer(q):
            total = coef[c, q, 0][None, :] * parts[0]
            for p in range(1, devices):
                total = total + coef[c, q, p][None, :] * parts[p]
            return total

        def merge(one, two):
            return jnp.where(keep, one, two) + pltpu.roll(jnp.where(keep, two, one), half, 1)

        def pair(i):
            here = merge(outer(2 * i), outer(2 * i + 1))
            there = merge(outer(2 * devices - 1 - 2 * i), outer(2 * devices - 2 - 2 * i))
            stacked = jnp.concatenate(
                [
                    jnp.concatenate([here, there * sign], axis=0),
                    jnp.concatenate([there, here * sign], axis=0),
                ],
                axis=1,
            ).astype(bf16)
            moved = jnp.dot(perm[...], stacked, preferred_element_type=f32).astype(bf16)
            send3[c, i] = moved[:, :group]
            send3[c, devices - 1 - i] = moved[:, group:]

        if devices <= 8:
            for i in range(wing):
                pair(i)
        else:
            each(pair, wing)

        def start3(d):
            to = target(d)
            exchange3(c, to, me).start()

            @pl.when(near(to))
            def _():
                for j in range(1, chips):
                    if c:
                        direct(0, j, to).wait_send()
                    direct(c, j, to).start()

        each(start3)
        recv3[c, col, me] = send3[c, me]

    combine(0)
    combine(1)

    def to_partner(c, g, src):
        block = recv3.at[c, g, src]
        return remote(block, block, psem.at[g, src], gsem.at[c, g, src], {"col": partner})

    def to_chip(c, j, g, src):
        block = recv3.at[c, g, src]
        return remote(block, block, ysem.at[j, src], gsem.at[c, g, src], {"col": peer_col(j)})

    def forward(c, src):
        @pl.when(jnp.logical_or(src == me, jnp.logical_not(near(src))))
        def _():
            for j in range(1, chips):
                if c:
                    to_chip(0, j, col, src).wait_send()
                to_chip(c, j, col, src).start()

        if c:
            to_partner(0, col, src).wait_send()
        to_partner(c, col, src).start()

    def relay(c, src):
        for j in range(1, chips):
            g = lax.rem(col + cols - 2 * j, cols)
            to_chip(c, j, g, src).wait_recv()
            if c:
                to_partner(0, g, src).wait_send()
            to_partner(c, g, src).start()

    def pass_on(c, src):
        exchange3(c, me, src).wait_recv()
        forward(c, src)

    def collect(c, src):
        for j in range(chips):
            to_partner(c, lax.rem(partner + 2 * j, cols), src).wait_recv()

    upper = me // wing
    mine = jnp.logical_xor(low, upper == 1)

    def finish(c, h):
        tiles = []
        for t in range(chips):
            one = recv3[c, 2 * t].reshape(devices * packet, group)
            two = recv3[c, 2 * t + 1].reshape(devices * packet, group)
            tiles.append(jnp.where(mine, two, one) if h else jnp.where(mine, one, two))
        arrived = jnp.concatenate(tiles, axis=1) if chips > 1 else tiles[0]
        natural = jnp.dot(order[...], arrived, preferred_element_type=f32).astype(bf16)
        which = 1 - upper if h else upper
        part = jnp.dot(natural, weight[which, c], preferred_element_type=f32)
        at = slice(h * period, (h + 1) * period)
        if c == 0:
            acc[at, :] = part
        else:
            out_ref[at, :] = (acc[at, :] + part).astype(bf16)

    forward(0, me)
    each(lambda d: pass_on(0, source(d)))
    forward(1, me)
    relay(0, me)

    def second(d):
        pass_on(1, source(d))
        relay(0, source(d))

    each(second)
    collect(0, me)
    each(lambda d: collect(0, source(d)))
    finish(0, 0)
    relay(1, me)
    each(lambda d: relay(1, source(d)))
    finish(0, 1)
    collect(1, me)
    each(lambda d: collect(1, source(d)))
    finish(1, 0)
    finish(1, 1)

    def drain(d):
        to = target(d)
        for r in range(subs):
            exchange1(r, to, me).wait_send()
        for c in range(2):
            exchange2(c, to, me).wait_send()
            exchange3(c, to, me).wait_send()

    each(drain)

    def drain_gather(src):
        aside = jnp.logical_and(src != me, near(src))

        @pl.when(jnp.logical_not(aside))
        def _():
            for j in range(1, chips):
                to_chip(1, j, col, src).wait_send()

        @pl.when(aside)
        def _():
            for j in range(1, chips):
                direct(1, j, src).wait_send()

        for j in range(chips):
            to_partner(1, peer_col(j), src).wait_send()

    each(drain_gather, devices)


def solution(mesh):
    devices, cols = mesh.shape["row"], mesh.shape["col"]

    def on_device(tokens, proj_in, proj_out):
        rows, width = tokens.shape
        group = proj_in.shape[1]
        channels, out_cols = proj_out.shape
        period, piece, subs, pad, share, height, packet = plan(rows, devices)
        consts = tables(rows, devices, group)
        chunks = 6
        f32, bf16 = jnp.float32, jnp.bfloat16
        dma = pltpu.SemaphoreType.DMA
        operands = [tokens, proj_in, proj_out, *[jnp.asarray(c) for c in consts]]
        return pl.pallas_call(
            functools.partial(kernel, devices, cols, chunks),
            out_shape=jax.ShapeDtypeStruct((rows, out_cols), bf16),
            in_specs=[pl.BlockSpec(memory_space=pltpu.HBM)] * len(operands),
            out_specs=pl.BlockSpec(memory_space=pltpu.VMEM),
            scratch_shapes=[
                pltpu.VMEM((rows, width), bf16),
                pltpu.VMEM((width, group), bf16),
                pltpu.VMEM((channels, out_cols), bf16),
                pltpu.VMEM(consts[0].shape, bf16),
                pltpu.VMEM((group, group), bf16),
                pltpu.VMEM(consts[2].shape[1:], bf16),
                pltpu.VMEM(consts[3].shape, f32),
                pltpu.VMEM(consts[4].shape, bf16),
                pltpu.VMEM(consts[5].shape, bf16),
                pltpu.VMEM((rows, group), f32),
                pltpu.VMEM((subs, devices, 2, pad, group), bf16),
                pltpu.VMEM((devices, subs, 2, pad, group), bf16),
                pltpu.VMEM((devices, 2 * height, 2 * group), f32),
                pltpu.VMEM((2, devices, height, group), bf16),
                pltpu.VMEM((2, devices, height, group), bf16),
                pltpu.VMEM((devices, height, group), f32),
                pltpu.VMEM((devices, height, group), f32),
                pltpu.VMEM((devices, height, group), f32),
                pltpu.VMEM((2, devices, packet, group), bf16),
                pltpu.VMEM((2, cols, devices, packet, group), bf16),
                pltpu.VMEM((2, 2, channels // 2, out_cols), bf16),
                pltpu.VMEM((rows, out_cols), f32),
                dma((chunks,)),
                dma((8,)),
                dma((subs, devices)),
                dma((subs, devices)),
                dma((2, devices)),
                dma((2, devices)),
                dma((2, devices)),
                dma((2, devices)),
                dma((2, cols, devices)),
                dma((cols // 2, devices)),
                dma((cols // 2, devices)),
                dma((cols, devices)),
            ],
            compiler_params=pltpu.CompilerParams(
                collective_id=0, has_side_effects=True, vmem_limit_bytes=44 * 2**20
            ),
            name="mix",
        )(*[pltpu.with_memory_space_constraint(a, pltpu.HBM) for a in operands])

    return jax.shard_map(
        on_device,
        mesh=mesh,
        in_specs=(P("row", None), P(None, "col"), P(None, "col")),
        out_specs=P("row", "col"),
        check_vma=False,
    )
```

```python
import functools
import math

import jax
import jax.numpy as jnp
import numpy as np
from jax import lax
from jax.experimental import pallas as pl
from jax.experimental.pallas import tpu as pltpu
from jax.sharding import PartitionSpec as P

MESH = pl.DeviceIdType.MESH


def up(value, step):
    return -(-value // step) * step


def plan(rows, devices):
    period = rows // 2
    piece = rows // (2 * devices)
    subs = 3 if piece % 24 == 0 else 1
    pad = up(piece // subs, 8)
    share = period // (2 * devices)
    height = up(share + 1, 8)
    packet = up(2 * share, 8)
    return period, piece, subs, pad, share, height, packet


@functools.lru_cache(maxsize=None)
def tables(rows, devices, group):
    period, piece, subs, pad, share, height, packet = plan(rows, devices)
    half = group // 2
    odd = np.arange(group) > half
    freq = np.where(odd, np.arange(group) - half, np.arange(group))
    angle = 2 * np.pi * (np.arange(group)[:, None] * freq[None, :] % group) / group
    chan = np.where(odd, np.sin(angle), np.cos(angle)) / math.sqrt(group)
    chan_hi = chan.astype(jnp.bfloat16)
    chan_lo = (chan - chan_hi.astype(np.float64)).astype(jnp.bfloat16)
    unpack = np.zeros((group, group))
    for col in range(group):
        f = freq[col]
        unpack[col, f] = -1.0 if odd[col] else 1.0
        unpack[col, (group - f) % group] = 1.0
    part = piece // subs
    pos = np.arange(2 * pad)
    is_y = pos >= pad
    local = np.where(is_y, pos - pad, pos)
    valid = np.tile(local < part, devices * subs)
    m = (
        part * np.arange(subs)[:, None, None]
        + piece * np.arange(devices)[None, :, None]
        + local[None, None, :]
    ).reshape(-1)
    is_y = np.tile(is_y, devices * subs)
    k = share * np.arange(devices)[:, None] + np.arange(height)[None, :]
    seq = []
    for twice_m in (2 * m + is_y, 2 * np.where(is_y, period - 1 - m, m)):
        angle = np.pi * (twice_m[None, None, :] * k[:, :, None] % (2 * period)) / period
        both = np.stack([np.cos(angle), np.sin(angle)], axis=1) * valid
        seq.append(both.reshape(devices * 2 * height, -1))
    seq = np.stack(seq).astype(jnp.bfloat16)
    q = np.arange(2 * devices)[:, None]
    p = np.arange(devices)[None, :]
    angle = 2 * np.pi * (p * q % (2 * devices)) / (2 * devices)
    even_a, even_b = np.cos(angle), -np.sin(angle)
    odd_a, odd_b = np.sin(angle), np.cos(angle)
    for a, b in ((even_a, even_b), (odd_a, odd_b)):
        a[:, 0] = 1.0
        b[:, 0] = np.where(q[:, 0] % 2, -1.0, 1.0)
    coef = []
    for c in range(2):
        is_odd = odd[c * half:(c + 1) * half]
        first = np.where(is_odd, odd_a[:, :, None], even_a[:, :, None])
        second = np.where(is_odd, odd_b[:, :, None], even_b[:, :, None])
        coef.append(np.concatenate([first, second], axis=2))
    coef = np.stack(coef) / math.sqrt(rows * devices)
    perm = np.zeros((packet, 2 * height))
    for j in range(share):
        perm[j, j] = 1.0
        perm[share + j, height + share - j] = 1.0
    return (
        np.concatenate([chan_hi, chan_lo], axis=0),
        unpack.astype(jnp.bfloat16),
        seq,
        coef.astype(np.float32),
        perm.astype(jnp.bfloat16),
    )


def cos_sin_small(x):
    square = x * x
    cos_sum, sin_sum = jnp.zeros_like(x), jnp.zeros_like(x)
    for j in range(8, -1, -1):
        sign = -1.0 if j % 2 else 1.0
        cos_sum = cos_sum * square + sign / math.factorial(2 * j)
        sin_sum = sin_sum * square + sign / math.factorial(2 * j + 1)
    return cos_sum, sin_sum * x


def kernel(
    devices, cols, chunks,
    tok_hbm, pin_hbm, pout_hbm, chan_hbm, unpack_hbm, seq_hbm, coef_hbm, perm_hbm,
    out_ref,
    tok, pin, pout, chan, unpack, seq, coef, perm,
    packed, send1, recv1, mid, send2, recv2, twc, tws, parts, send3, recv3, weight, acc,
    tok_sem, in_sem, ssem1, rsem1, ssem2, rsem2, ssem3, rsem3, gsem, ysem, nsem, psem,
):
    me = lax.axis_index("row")
    col = lax.axis_index("col")
    partner = col + 1 - 2 * lax.rem(col, 2)
    rows, group = packed.shape
    period, piece, subs, pad, share, height, packet = plan(rows, devices)
    half = group // 2
    f32, bf16 = jnp.float32, jnp.bfloat16
    chips = cols // 2
    wing = devices // 2

    def target(d):
        return lax.rem(me + 1 + d, devices)

    def source(d):
        return lax.rem(me + devices - 1 - d, devices)

    def peer_col(j):
        return lax.rem(col + 2 * j, cols)

    def near(row):
        return row // wing == me // wing

    def each(body, count=devices - 1, unroll=False):
        def step(d, _):
            body(d)
            return 0

        lax.fori_loop(0, count, step, 0, unroll=unroll)

    barrier = pltpu.get_barrier_semaphore()

    step = rows // chunks
    depth = chunks // 2
    tok_copies = [
        pltpu.make_async_copy(
            tok_hbm.at[pl.ds(i * step, step)], tok.at[pl.ds(i * step, step)], tok_sem.at[i]
        )
        for i in range(chunks)
    ]
    loads = [
        pltpu.make_async_copy(src, dst, in_sem.at[i])
        for i, (src, dst) in enumerate(
            [
                (pin_hbm, pin),
                (chan_hbm, chan),
                (pout_hbm, pout),
                (unpack_hbm, unpack),
                (seq_hbm.at[jnp.minimum(me, 1)], seq),
                (coef_hbm, coef),
                (perm_hbm, perm),
            ]
        )
    ]
    loads[0].start()
    tok_copies[0].start()
    loads[1].start()
    for copy in tok_copies[1:depth]:
        copy.start()
    each(lambda d: pl.semaphore_signal(
        barrier, inc=1, device_id={"row": target(d)}, device_id_type=MESH
    ))
    pl.semaphore_signal(barrier, inc=1, device_id={"col": partner}, device_id_type=MESH)
    for j in range(1, chips):
        pl.semaphore_signal(barrier, inc=1, device_id={"col": peer_col(j)}, device_id_type=MESH)

    def greet(d):
        @pl.when(near(target(d)))
        def _():
            for j in range(1, chips):
                pl.semaphore_signal(
                    barrier, inc=1, device_id={"row": target(d), "col": peer_col(j)},
                    device_id_type=MESH,
                )

    each(greet)

    lane = lax.broadcasted_iota(jnp.int32, (1, group), 1)
    low = lane < half

    shape = (devices, height, group)
    p_id = lax.broadcasted_iota(jnp.int32, shape, 0)
    k_id = lax.broadcasted_iota(jnp.int32, shape, 1) + share * me
    angle = (p_id * k_id).astype(f32) * (2.0 * math.pi / (rows * devices))
    cos_val, sin_val = cos_sin_small(angle)
    twc[...] = cos_val
    tws[...] = jnp.where(low, -sin_val, sin_val)

    def sign_of(channel):
        return jnp.where(channel > half, -1.0, 1.0).astype(f32)

    y_sign = sign_of(lane)

    def remote(src, dst, ssem, rsem, to):
        return pltpu.make_async_remote_copy(
            src_ref=src, dst_ref=dst, send_sem=ssem, recv_sem=rsem,
            device_id=to, device_id_type=MESH,
        )

    def exchange1(r, to, slot):
        return remote(
            send1.at[r, to], recv1.at[slot, r], ssem1.at[r, to], rsem1.at[r, slot], {"row": to}
        )

    part = piece // subs
    per_sub = chunks // subs
    if pad != part:
        send1[...] = jnp.zeros_like(send1)
    loads[0].wait()
    for i in range(chunks):
        tok_copies[i].wait()
        if i + depth < chunks:
            tok_copies[i + depth].start()
        elif i + depth == chunks:
            for copy in loads[2:]:
                copy.start()
        branch = jnp.dot(
            tok[i * step:(i + 1) * step, :], pin[...], preferred_element_type=f32
        ).astype(bf16)
        if i == 0:
            loads[1].wait()
        packed[i * step:(i + 1) * step, :] = jnp.dot(
            jnp.concatenate([branch, branch], axis=1), chan[...], preferred_element_type=f32
        )
        if (i + 1) % per_sub:
            continue
        r = i // per_sub
        base = r * (rows // subs)
        for p in range(devices):
            other = 2 * devices - p if p else devices
            y = packed[pl.ds(base + other, part, stride=2 * devices), :]
            if p:
                y = y * y_sign
            x = packed[pl.ds(base + p, part, stride=2 * devices), :]
            send1[r, p, 0, 0:part, :] = x.astype(bf16)
            send1[r, p, 1, 0:part, :] = y.astype(bf16)
        if r == 0:
            pl.semaphore_wait(barrier, devices + (chips - 1) * wing)
        each(lambda d: exchange1(r, target(d), me).start())
    for r in range(subs):
        recv1[me, r] = send1[r, me]

    for copy in loads[2:]:
        copy.wait()
    for g in range(cols):
        unpacked = jnp.dot(
            unpack[...], pout[g * group:(g + 1) * group, :], preferred_element_type=f32
        ).astype(bf16)
        top = g // 2 * group
        for v in range(2):
            at = top + (half if (g + v) % 2 else 0)
            for c in range(2):
                weight[v, c, at:at + half, :] = unpacked[c * half:(c + 1) * half, :]

    first = me == 0

    def exchange2(c, to, slot):
        return remote(
            send2.at[c, to], recv2.at[c, slot], ssem2.at[c, to], rsem2.at[c, slot], {"row": to}
        )

    def channel_of(c):
        return c * half + lax.rem(lane, half)

    odd_lane = lane > half
    span = devices * 2 * pad
    for r in range(subs):
        each(lambda d: exchange1(r, me, source(d)).wait_recv())
        data = recv1[:, r]
        blank = jnp.zeros_like(data[:, 0])
        both = jnp.concatenate(
            [
                jnp.stack([data[:, 0], blank], axis=1).reshape(span, group),
                jnp.stack([blank, data[:, 1]], axis=1).reshape(span, group),
            ],
            axis=1,
        )
        term = jnp.dot(
            seq[:, r * span:(r + 1) * span], both, preferred_element_type=f32
        ).reshape(mid.shape)
        mid[...] = mid[...] + term if r else term

    def fill(s):
        top_x, top_y = mid[s, :height, :group], mid[s, :height, group:]
        low_x, low_y = mid[s, height:, :group], mid[s, height:, group:]
        a = jnp.where(first, jnp.where(odd_lane, low_x, top_x), top_x + top_y)
        b = jnp.where(first, jnp.where(odd_lane, low_y, top_y), low_x + low_y)
        send2[0, s] = jnp.where(low, a, pltpu.roll(b, half, 1)).astype(bf16)
        send2[1, s] = jnp.where(low, pltpu.roll(a, half, 1), b).astype(bf16)

    def start2(d):
        fill(target(d))
        exchange2(0, target(d), me).start()

    each(start2, unroll=devices <= 8)
    each(lambda d: exchange2(1, target(d), me).start())
    fill(me)
    recv2[0, me] = send2[0, me]
    recv2[1, me] = send2[1, me]

    def exchange3(c, to, slot):
        return remote(
            send3.at[c, to], recv3.at[c, col, slot], ssem3.at[c, to], rsem3.at[c, slot],
            {"row": to},
        )

    def direct(c, j, to):
        return remote(
            send3.at[c, to], recv3.at[c, col, me], nsem.at[j, to], gsem.at[c, col, me],
            {"row": to, "col": peer_col(j)},
        )

    keep = jnp.logical_xor(low, lax.rem(col, 2) == 1)

    def combine(c):
        def rotate(src):
            value = recv2[c, src].astype(f32)
            parts[src] = twc[src] * value + tws[src] * pltpu.roll(value, half, 1)

        rotate(me)

        def arrive(d):
            exchange2(c, me, source(d)).wait_recv()
            rotate(source(d))

        each(arrive, unroll=devices <= 8)
        sign = sign_of(channel_of(c))

        def outer(q):
            total = coef[c, q, 0][None, :] * parts[0]
            for p in range(1, devices):
                total = total + coef[c, q, p][None, :] * parts[p]
            return total

        def merge(one, two):
            return jnp.where(keep, one, two) + pltpu.roll(jnp.where(keep, two, one), half, 1)

        def pair(i):
            here = merge(outer(2 * i), outer(2 * i + 1))
            there = merge(outer(2 * devices - 1 - 2 * i), outer(2 * devices - 2 - 2 * i))
            stacked = jnp.concatenate(
                [
                    jnp.concatenate([here, there * sign], axis=0),
                    jnp.concatenate([there, here * sign], axis=0),
                ],
                axis=1,
            ).astype(bf16)
            moved = jnp.dot(perm[...], stacked, preferred_element_type=f32).astype(bf16)
            send3[c, i] = moved[:, :group]
            send3[c, devices - 1 - i] = moved[:, group:]

        if devices <= 8:
            for i in range(wing):
                pair(i)
        else:
            each(pair, wing)

        def start3(d):
            to = target(d)
            exchange3(c, to, me).start()

            @pl.when(near(to))
            def _():
                for j in range(1, chips):
                    if c:
                        direct(0, j, to).wait_send()
                    direct(c, j, to).start()

        each(start3)
        recv3[c, col, me] = send3[c, me]

    combine(0)
    combine(1)

    def to_partner(c, g, src):
        block = recv3.at[c, g, src]
        return remote(block, block, psem.at[g, src], gsem.at[c, g, src], {"col": partner})

    def to_chip(c, j, g, src):
        block = recv3.at[c, g, src]
        return remote(block, block, ysem.at[j, src], gsem.at[c, g, src], {"col": peer_col(j)})

    def forward(c, src):
        @pl.when(jnp.logical_or(src == me, jnp.logical_not(near(src))))
        def _():
            for j in range(1, chips):
                if c:
                    to_chip(0, j, col, src).wait_send()
                to_chip(c, j, col, src).start()

        if c:
            to_partner(0, col, src).wait_send()
        to_partner(c, col, src).start()

    def relay(c, src):
        for j in range(1, chips):
            g = lax.rem(col + cols - 2 * j, cols)
            to_chip(c, j, g, src).wait_recv()
            if c:
                to_partner(0, g, src).wait_send()
            to_partner(c, g, src).start()

    def pass_on(c, src):
        exchange3(c, me, src).wait_recv()
        forward(c, src)

    def collect(c, src):
        for j in range(chips):
            to_partner(c, lax.rem(partner + 2 * j, cols), src).wait_recv()

    upper = me // wing
    mine = jnp.logical_xor(low, upper == 1)

    def finish(c):
        tiles = []
        for h in range(2):
            for t in range(chips):
                one = recv3[c, 2 * t].reshape(devices * packet, group)
                two = recv3[c, 2 * t + 1].reshape(devices * packet, group)
                tiles.append(jnp.where(mine, two, one) if h else jnp.where(mine, one, two))
        lined = jnp.concatenate(tiles, axis=1).astype(f32).reshape(devices, packet, -1)
        natural = jnp.concatenate(
            [lined[p, :share] for p in range(devices)]
            + [lined[p, share:2 * share] for p in range(devices - 1, -1, -1)],
            axis=0,
        ).astype(bf16)
        for h in range(2):
            which = 1 - upper if h else upper
            part = jnp.dot(
                natural[:, h * chips * group:(h + 1) * chips * group], weight[which, c],
                preferred_element_type=f32,
            )
            at = slice(h * period, (h + 1) * period)
            if c == 0:
                acc[at, :] = part
            else:
                out_ref[at, :] = (acc[at, :] + part).astype(bf16)

    forward(0, me)
    each(lambda d: pass_on(0, source(d)))
    forward(1, me)
    relay(0, me)

    def second(d):
        pass_on(1, source(d))
        relay(0, source(d))

    each(second)
    collect(0, me)
    each(lambda d: collect(0, source(d)))
    finish(0)
    relay(1, me)
    each(lambda d: relay(1, source(d)))
    collect(1, me)
    each(lambda d: collect(1, source(d)))
    finish(1)

    def drain(d):
        to = target(d)
        for r in range(subs):
            exchange1(r, to, me).wait_send()
        for c in range(2):
            exchange2(c, to, me).wait_send()
            exchange3(c, to, me).wait_send()

    each(drain)

    def drain_gather(src):
        aside = jnp.logical_and(src != me, near(src))

        @pl.when(jnp.logical_not(aside))
        def _():
            for j in range(1, chips):
                to_chip(1, j, col, src).wait_send()

        @pl.when(aside)
        def _():
            for j in range(1, chips):
                direct(1, j, src).wait_send()

        for j in range(chips):
            to_partner(1, peer_col(j), src).wait_send()

    each(drain_gather, devices)


def solution(mesh):
    devices, cols = mesh.shape["row"], mesh.shape["col"]

    def on_device(tokens, proj_in, proj_out):
        rows, width = tokens.shape
        group = proj_in.shape[1]
        channels, out_cols = proj_out.shape
        period, piece, subs, pad, share, height, packet = plan(rows, devices)
        consts = tables(rows, devices, group)
        chunks = 6
        f32, bf16 = jnp.float32, jnp.bfloat16
        dma = pltpu.SemaphoreType.DMA
        operands = [tokens, proj_in, proj_out, *[jnp.asarray(c) for c in consts]]
        return pl.pallas_call(
            functools.partial(kernel, devices, cols, chunks),
            out_shape=jax.ShapeDtypeStruct((rows, out_cols), bf16),
            in_specs=[pl.BlockSpec(memory_space=pltpu.HBM)] * len(operands),
            out_specs=pl.BlockSpec(memory_space=pltpu.VMEM),
            scratch_shapes=[
                pltpu.VMEM((rows, width), bf16),
                pltpu.VMEM((width, group), bf16),
                pltpu.VMEM((channels, out_cols), bf16),
                pltpu.VMEM(consts[0].shape, bf16),
                pltpu.VMEM((group, group), bf16),
                pltpu.VMEM(consts[2].shape[1:], bf16),
                pltpu.VMEM(consts[3].shape, f32),
                pltpu.VMEM(consts[4].shape, bf16),
                pltpu.VMEM((rows, group), f32),
                pltpu.VMEM((subs, devices, 2, pad, group), bf16),
                pltpu.VMEM((devices, subs, 2, pad, group), bf16),
                pltpu.VMEM((devices, 2 * height, 2 * group), f32),
                pltpu.VMEM((2, devices, height, group), bf16),
                pltpu.VMEM((2, devices, height, group), bf16),
                pltpu.VMEM((devices, height, group), f32),
                pltpu.VMEM((devices, height, group), f32),
                pltpu.VMEM((devices, height, group), f32),
                pltpu.VMEM((2, devices, packet, group), bf16),
                pltpu.VMEM((2, cols, devices, packet, group), bf16),
                pltpu.VMEM((2, 2, channels // 2, out_cols), bf16),
                pltpu.VMEM((rows, out_cols), f32),
                dma((chunks,)),
                dma((7,)),
                dma((subs, devices)),
                dma((subs, devices)),
                dma((2, devices)),
                dma((2, devices)),
                dma((2, devices)),
                dma((2, devices)),
                dma((2, cols, devices)),
                dma((cols // 2, devices)),
                dma((cols // 2, devices)),
                dma((cols, devices)),
            ],
            compiler_params=pltpu.CompilerParams(
                collective_id=0, has_side_effects=True, vmem_limit_bytes=44 * 2**20
            ),
            name="mix",
        )(*[pltpu.with_memory_space_constraint(a, pltpu.HBM) for a in operands])

    return jax.shard_map(
        on_device,
        mesh=mesh,
        in_specs=(P("row", None), P(None, "col"), P(None, "col")),
        out_specs=P("row", "col"),
        check_vma=False,
    )
```

```python
import functools
import math

import jax
import jax.numpy as jnp
import numpy as np
from jax import lax
from jax.experimental import pallas as pl
from jax.experimental.pallas import tpu as pltpu
from jax.sharding import PartitionSpec as P

MESH = pl.DeviceIdType.MESH


def up(value, step):
    return -(-value // step) * step


def plan(rows, devices):
    period = rows // 2
    piece = rows // (2 * devices)
    subs = 3 if piece % 24 == 0 else 1
    pad = up(piece // subs, 8)
    share = period // (2 * devices)
    height = up(share + 1, 8)
    packet = up(2 * share, 8)
    return period, piece, subs, pad, share, height, packet


@functools.lru_cache(maxsize=None)
def tables(rows, devices, group):
    period, piece, subs, pad, share, height, packet = plan(rows, devices)
    half = group // 2
    odd = np.arange(group) > half
    freq = np.where(odd, np.arange(group) - half, np.arange(group))
    angle = 2 * np.pi * (np.arange(group)[:, None] * freq[None, :] % group) / group
    chan = np.where(odd, np.sin(angle), np.cos(angle)) / math.sqrt(group)
    chan_hi = chan.astype(jnp.bfloat16)
    chan_lo = (chan - chan_hi.astype(np.float64)).astype(jnp.bfloat16)
    unpack = np.zeros((group, group))
    for col in range(group):
        f = freq[col]
        unpack[col, f] = -1.0 if odd[col] else 1.0
        unpack[col, (group - f) % group] = 1.0
    part = piece // subs
    pos = np.arange(2 * pad)
    is_y = pos >= pad
    local = np.where(is_y, pos - pad, pos)
    valid = np.tile(local < part, devices * subs)
    m = (
        part * np.arange(subs)[:, None, None]
        + piece * np.arange(devices)[None, :, None]
        + local[None, None, :]
    ).reshape(-1)
    is_y = np.tile(is_y, devices * subs)
    k = share * np.arange(devices)[:, None] + np.arange(height)[None, :]
    seq = []
    for twice_m in (2 * m + is_y, 2 * np.where(is_y, period - 1 - m, m)):
        angle = np.pi * (twice_m[None, None, :] * k[:, :, None] % (2 * period)) / period
        both = np.stack([np.cos(angle), np.sin(angle)], axis=1) * valid
        seq.append(both.reshape(devices * 2 * height, -1))
    seq = np.stack(seq).astype(jnp.bfloat16)
    q = np.arange(2 * devices)[:, None]
    p = np.arange(devices)[None, :]
    angle = 2 * np.pi * (p * q % (2 * devices)) / (2 * devices)
    even_a, even_b = np.cos(angle), -np.sin(angle)
    odd_a, odd_b = np.sin(angle), np.cos(angle)
    for a, b in ((even_a, even_b), (odd_a, odd_b)):
        a[:, 0] = 1.0
        b[:, 0] = np.where(q[:, 0] % 2, -1.0, 1.0)
    coef = []
    for c in range(2):
        is_odd = odd[c * half:(c + 1) * half]
        first = np.where(is_odd, odd_a[:, :, None], even_a[:, :, None])
        second = np.where(is_odd, odd_b[:, :, None], even_b[:, :, None])
        coef.append(np.concatenate([first, second], axis=2))
    coef = np.stack(coef) / math.sqrt(rows * devices)
    perm = np.zeros((packet, 2 * height))
    for j in range(share):
        perm[j, j] = 1.0
        perm[share + j, height + share - j] = 1.0
    return (
        np.concatenate([chan_hi, chan_lo], axis=0),
        unpack.astype(jnp.bfloat16),
        seq,
        coef.astype(np.float32),
        perm.astype(jnp.bfloat16),
    )


def cos_sin_small(x):
    square = x * x
    cos_sum, sin_sum = jnp.zeros_like(x), jnp.zeros_like(x)
    for j in range(8, -1, -1):
        sign = -1.0 if j % 2 else 1.0
        cos_sum = cos_sum * square + sign / math.factorial(2 * j)
        sin_sum = sin_sum * square + sign / math.factorial(2 * j + 1)
    return cos_sum, sin_sum * x


def kernel(
    devices, cols, chunks,
    tok_hbm, pin_hbm, pout_hbm, chan_hbm, unpack_hbm, seq_hbm, coef_hbm, perm_hbm,
    out_ref,
    tok, pin, pout, chan, unpack, seq, coef, perm,
    packed, send1, recv1, mid, send2, recv2, twc, tws, parts, send3, recv3, weight, acc,
    tok_sem, in_sem, ssem1, rsem1, ssem2, rsem2, ssem3, rsem3, gsem, ysem, nsem, psem,
):
    me = lax.axis_index("row")
    col = lax.axis_index("col")
    partner = col + 1 - 2 * lax.rem(col, 2)
    rows, group = packed.shape
    period, piece, subs, pad, share, height, packet = plan(rows, devices)
    half = group // 2
    f32, bf16 = jnp.float32, jnp.bfloat16
    chips = cols // 2
    wing = devices // 2

    def target(d):
        return lax.rem(me + 1 + d, devices)

    def source(d):
        return lax.rem(me + devices - 1 - d, devices)

    def peer_col(j):
        return lax.rem(col + 2 * j, cols)

    def near(row):
        return row // wing == me // wing

    def each(body, count=devices - 1, unroll=False):
        def step(d, _):
            body(d)
            return 0

        lax.fori_loop(0, count, step, 0, unroll=unroll)

    barrier = pltpu.get_barrier_semaphore()

    step = rows // chunks
    depth = chunks // 2
    tok_copies = [
        pltpu.make_async_copy(
            tok_hbm.at[pl.ds(i * step, step)], tok.at[pl.ds(i * step, step)], tok_sem.at[i]
        )
        for i in range(chunks)
    ]
    loads = [
        pltpu.make_async_copy(src, dst, in_sem.at[i])
        for i, (src, dst) in enumerate(
            [
                (pin_hbm, pin),
                (chan_hbm, chan),
                (pout_hbm, pout),
                (unpack_hbm, unpack),
                (seq_hbm.at[jnp.minimum(me, 1)], seq),
                (coef_hbm, coef),
                (perm_hbm, perm),
            ]
        )
    ]
    loads[0].start()
    tok_copies[0].start()
    loads[1].start()
    for copy in tok_copies[1:depth]:
        copy.start()
    each(lambda d: pl.semaphore_signal(
        barrier, inc=1, device_id={"row": target(d)}, device_id_type=MESH
    ))
    pl.semaphore_signal(barrier, inc=1, device_id={"col": partner}, device_id_type=MESH)
    for j in range(1, chips):
        pl.semaphore_signal(barrier, inc=1, device_id={"col": peer_col(j)}, device_id_type=MESH)

    def greet(d):
        @pl.when(near(target(d)))
        def _():
            for j in range(1, chips):
                pl.semaphore_signal(
                    barrier, inc=1, device_id={"row": target(d), "col": peer_col(j)},
                    device_id_type=MESH,
                )

    each(greet)

    lane = lax.broadcasted_iota(jnp.int32, (1, group), 1)
    low = lane < half

    shape = (devices, height, group)
    p_id = lax.broadcasted_iota(jnp.int32, shape, 0)
    k_id = lax.broadcasted_iota(jnp.int32, shape, 1) + share * me
    angle = (p_id * k_id).astype(f32) * (2.0 * math.pi / (rows * devices))
    cos_val, sin_val = cos_sin_small(angle)
    twc[...] = cos_val
    tws[...] = jnp.where(low, -sin_val, sin_val)

    def sign_of(channel):
        return jnp.where(channel > half, -1.0, 1.0).astype(f32)

    y_sign = sign_of(lane)

    def remote(src, dst, ssem, rsem, to):
        return pltpu.make_async_remote_copy(
            src_ref=src, dst_ref=dst, send_sem=ssem, recv_sem=rsem,
            device_id=to, device_id_type=MESH,
        )

    def exchange1(r, to, slot):
        return remote(
            send1.at[r, to], recv1.at[slot, r], ssem1.at[r, to], rsem1.at[r, slot], {"row": to}
        )

    part = piece // subs
    per_sub = chunks // subs
    if pad != part:
        send1[...] = jnp.zeros_like(send1)
    loads[0].wait()
    for i in range(chunks):
        tok_copies[i].wait()
        if i + depth < chunks:
            tok_copies[i + depth].start()
        elif i + depth == chunks:
            for copy in loads[2:]:
                copy.start()
        branch = jnp.dot(
            tok[i * step:(i + 1) * step, :], pin[...], preferred_element_type=f32
        ).astype(bf16)
        if i == 0:
            loads[1].wait()
        packed[i * step:(i + 1) * step, :] = jnp.dot(
            jnp.concatenate([branch, branch], axis=1), chan[...], preferred_element_type=f32
        )
        if (i + 1) % per_sub:
            continue
        r = i // per_sub
        base = r * (rows // subs)
        for p in range(devices):
            other = 2 * devices - p if p else devices
            y = packed[pl.ds(base + other, part, stride=2 * devices), :]
            if p:
                y = y * y_sign
            x = packed[pl.ds(base + p, part, stride=2 * devices), :]
            send1[r, p, 0, 0:part, :] = x.astype(bf16)
            send1[r, p, 1, 0:part, :] = y.astype(bf16)
        if r == 0:
            pl.semaphore_wait(barrier, devices + (chips - 1) * wing)
        each(lambda d: exchange1(r, target(d), me).start())
    for r in range(subs):
        recv1[me, r] = send1[r, me]

    for copy in loads[2:]:
        copy.wait()

    def mix_weight(t):
        for b in range(2):
            g_at = pl.ds(pl.multiple_of((2 * t + b) * group, group), group)
            unpacked = jnp.dot(
                unpack[...], pout[g_at, :], preferred_element_type=f32
            ).astype(bf16)
            for v in range(2):
                at = pl.ds(pl.multiple_of(t * group + half * ((b + v) % 2), half), half)
                for c in range(2):
                    weight[v, c, at, :] = unpacked[c * half:(c + 1) * half, :]

    each(mix_weight, chips)

    first = me == 0

    def exchange2(c, to, slot):
        return remote(
            send2.at[c, to], recv2.at[c, slot], ssem2.at[c, to], rsem2.at[c, slot], {"row": to}
        )

    def channel_of(c):
        return c * half + lax.rem(lane, half)

    odd_lane = lane > half
    span = devices * 2 * pad
    for r in range(subs):
        each(lambda d: exchange1(r, me, source(d)).wait_recv())
        data = recv1[:, r]
        blank = jnp.zeros_like(data[:, 0])
        both = jnp.concatenate(
            [
                jnp.stack([data[:, 0], blank], axis=1).reshape(span, group),
                jnp.stack([blank, data[:, 1]], axis=1).reshape(span, group),
            ],
            axis=1,
        )
        term = jnp.dot(
            seq[:, r * span:(r + 1) * span], both, preferred_element_type=f32
        ).reshape(mid.shape)
        mid[...] = mid[...] + term if r else term

    def fill(s):
        top_x, top_y = mid[s, :height, :group], mid[s, :height, group:]
        low_x, low_y = mid[s, height:, :group], mid[s, height:, group:]
        a = jnp.where(first, jnp.where(odd_lane, low_x, top_x), top_x + top_y)
        b = jnp.where(first, jnp.where(odd_lane, low_y, top_y), low_x + low_y)
        send2[0, s] = jnp.where(low, a, pltpu.roll(b, half, 1)).astype(bf16)
        send2[1, s] = jnp.where(low, pltpu.roll(a, half, 1), b).astype(bf16)

    def start2(d):
        fill(target(d))
        exchange2(0, target(d), me).start()

    each(start2)
    each(lambda d: exchange2(1, target(d), me).start())
    fill(me)
    recv2[0, me] = send2[0, me]
    recv2[1, me] = send2[1, me]

    def exchange3(c, to, slot):
        return remote(
            send3.at[c, to], recv3.at[c, col, slot], ssem3.at[c, to], rsem3.at[c, slot],
            {"row": to},
        )

    def direct(c, j, to):
        return remote(
            send3.at[c, to], recv3.at[c, col, me], nsem.at[j, to], gsem.at[c, col, me],
            {"row": to, "col": peer_col(j)},
        )

    keep = jnp.logical_xor(low, lax.rem(col, 2) == 1)

    def combine(c):
        def rotate(src):
            value = recv2[c, src].astype(f32)
            parts[src] = twc[src] * value + tws[src] * pltpu.roll(value, half, 1)

        rotate(me)

        def arrive(d):
            exchange2(c, me, source(d)).wait_recv()
            rotate(source(d))

        each(arrive)
        sign = sign_of(channel_of(c))

        def outer(q):
            total = coef[c, q, 0][None, :] * parts[0]
            for p in range(1, devices):
                total = total + coef[c, q, p][None, :] * parts[p]
            return total

        def merge(one, two):
            return jnp.where(keep, one, two) + pltpu.roll(jnp.where(keep, two, one), half, 1)

        def pair(i):
            here = merge(outer(2 * i), outer(2 * i + 1))
            there = merge(outer(2 * devices - 1 - 2 * i), outer(2 * devices - 2 - 2 * i))
            stacked = jnp.concatenate(
                [
                    jnp.concatenate([here, there * sign], axis=0),
                    jnp.concatenate([there, here * sign], axis=0),
                ],
                axis=1,
            ).astype(bf16)
            moved = jnp.dot(perm[...], stacked, preferred_element_type=f32).astype(bf16)
            send3[c, i] = moved[:, :group]
            send3[c, devices - 1 - i] = moved[:, group:]

        if devices <= 8:
            for i in range(wing):
                pair(i)
        else:
            each(pair, wing)

        def start3(d):
            to = target(d)
            exchange3(c, to, me).start()

            @pl.when(near(to))
            def _():
                for j in range(1, chips):
                    if c:
                        direct(0, j, to).wait_send()
                    direct(c, j, to).start()

        each(start3)
        recv3[c, col, me] = send3[c, me]

    combine(0)
    combine(1)

    def to_partner(c, g, src):
        block = recv3.at[c, g, src]
        return remote(block, block, psem.at[g, src], gsem.at[c, g, src], {"col": partner})

    def to_chip(c, j, g, src):
        block = recv3.at[c, g, src]
        return remote(block, block, ysem.at[j, src], gsem.at[c, g, src], {"col": peer_col(j)})

    def forward(c, src):
        @pl.when(jnp.logical_or(src == me, jnp.logical_not(near(src))))
        def _():
            for j in range(1, chips):
                if c:
                    to_chip(0, j, col, src).wait_send()
                to_chip(c, j, col, src).start()

        if c:
            to_partner(0, col, src).wait_send()
        to_partner(c, col, src).start()

    def relay(c, src):
        for j in range(1, chips):
            g = lax.rem(col + cols - 2 * j, cols)
            to_chip(c, j, g, src).wait_recv()
            if c:
                to_partner(0, g, src).wait_send()
            to_partner(c, g, src).start()

    def pass_on(c, src):
        exchange3(c, me, src).wait_recv()
        forward(c, src)

    def collect(c, src):
        for j in range(chips):
            to_partner(c, lax.rem(partner + 2 * j, cols), src).wait_recv()

    upper = me // wing
    mine = jnp.logical_xor(low, upper == 1)

    def finish(c):
        tiles = []
        for h in range(2):
            for t in range(chips):
                one = recv3[c, 2 * t].reshape(devices * packet, group)
                two = recv3[c, 2 * t + 1].reshape(devices * packet, group)
                tiles.append(jnp.where(mine, two, one) if h else jnp.where(mine, one, two))
        lined = jnp.concatenate(tiles, axis=1).astype(f32).reshape(devices, packet, -1)
        natural = jnp.concatenate(
            [lined[p, :share] for p in range(devices)]
            + [lined[p, share:2 * share] for p in range(devices - 1, -1, -1)],
            axis=0,
        ).astype(bf16)
        for h in range(2):
            which = 1 - upper if h else upper
            part = jnp.dot(
                natural[:, h * chips * group:(h + 1) * chips * group], weight[which, c],
                preferred_element_type=f32,
            )
            at = slice(h * period, (h + 1) * period)
            if c == 0:
                acc[at, :] = part
            else:
                out_ref[at, :] = (acc[at, :] + part).astype(bf16)

    forward(0, me)
    each(lambda d: pass_on(0, source(d)))
    forward(1, me)
    relay(0, me)

    def second(d):
        pass_on(1, source(d))
        relay(0, source(d))

    each(second)
    collect(0, me)
    each(lambda d: collect(0, source(d)))
    finish(0)
    relay(1, me)
    each(lambda d: relay(1, source(d)))
    collect(1, me)
    each(lambda d: collect(1, source(d)))
    finish(1)

    def drain(d):
        to = target(d)
        for r in range(subs):
            exchange1(r, to, me).wait_send()
        for c in range(2):
            exchange2(c, to, me).wait_send()
            exchange3(c, to, me).wait_send()

    each(drain)

    def drain_gather(src):
        aside = jnp.logical_and(src != me, near(src))

        @pl.when(jnp.logical_not(aside))
        def _():
            for j in range(1, chips):
                to_chip(1, j, col, src).wait_send()

        @pl.when(aside)
        def _():
            for j in range(1, chips):
                direct(1, j, src).wait_send()

        for j in range(chips):
            to_partner(1, peer_col(j), src).wait_send()

    each(drain_gather, devices)


def solution(mesh):
    devices, cols = mesh.shape["row"], mesh.shape["col"]

    def on_device(tokens, proj_in, proj_out):
        rows, width = tokens.shape
        group = proj_in.shape[1]
        channels, out_cols = proj_out.shape
        period, piece, subs, pad, share, height, packet = plan(rows, devices)
        consts = tables(rows, devices, group)
        chunks = 6
        f32, bf16 = jnp.float32, jnp.bfloat16
        dma = pltpu.SemaphoreType.DMA
        operands = [tokens, proj_in, proj_out, *[jnp.asarray(c) for c in consts]]
        return pl.pallas_call(
            functools.partial(kernel, devices, cols, chunks),
            out_shape=jax.ShapeDtypeStruct((rows, out_cols), bf16),
            in_specs=[pl.BlockSpec(memory_space=pltpu.HBM)] * len(operands),
            out_specs=pl.BlockSpec(memory_space=pltpu.VMEM),
            scratch_shapes=[
                pltpu.VMEM((rows, width), bf16),
                pltpu.VMEM((width, group), bf16),
                pltpu.VMEM((channels, out_cols), bf16),
                pltpu.VMEM(consts[0].shape, bf16),
                pltpu.VMEM((group, group), bf16),
                pltpu.VMEM(consts[2].shape[1:], bf16),
                pltpu.VMEM(consts[3].shape, f32),
                pltpu.VMEM(consts[4].shape, bf16),
                pltpu.VMEM((rows, group), f32),
                pltpu.VMEM((subs, devices, 2, pad, group), bf16),
                pltpu.VMEM((devices, subs, 2, pad, group), bf16),
                pltpu.VMEM((devices, 2 * height, 2 * group), f32),
                pltpu.VMEM((2, devices, height, group), bf16),
                pltpu.VMEM((2, devices, height, group), bf16),
                pltpu.VMEM((devices, height, group), f32),
                pltpu.VMEM((devices, height, group), f32),
                pltpu.VMEM((devices, height, group), f32),
                pltpu.VMEM((2, devices, packet, group), bf16),
                pltpu.VMEM((2, cols, devices, packet, group), bf16),
                pltpu.VMEM((2, 2, channels // 2, out_cols), bf16),
                pltpu.VMEM((rows, out_cols), f32),
                dma((chunks,)),
                dma((7,)),
                dma((subs, devices)),
                dma((subs, devices)),
                dma((2, devices)),
                dma((2, devices)),
                dma((2, devices)),
                dma((2, devices)),
                dma((2, cols, devices)),
                dma((cols // 2, devices)),
                dma((cols // 2, devices)),
                dma((cols, devices)),
            ],
            compiler_params=pltpu.CompilerParams(
                collective_id=0, has_side_effects=True, vmem_limit_bytes=44 * 2**20
            ),
            name="mix",
        )(*[pltpu.with_memory_space_constraint(a, pltpu.HBM) for a in operands])

    return jax.shard_map(
        on_device,
        mesh=mesh,
        in_specs=(P("row", None), P(None, "col"), P(None, "col")),
        out_specs=P("row", "col"),
        check_vma=False,
    )
```
